32 devices in a mesh: rep: 2 (over x), fs: 8 (over z, y), tp: 2 (over core).
Axes of the slice: x: 2, y: 2, z: 4, core: 2. Of those that a mesh axis runs over, the one named last changes fastest.
Arguments:
- tokens: bfloat16 [4096, 2048], P(('rep', 'fs')), may hold values from -6 to 6
- first_gain: float32 [2048], replicated, may hold values from 0.1 to 1.9
- value_weight: float32 [2048, 1024], P('fs', 'tp'), may hold values from -0.125 to 0.125
- gate_weight: float32 [2048, 1024], P('fs', 'tp'), may hold values from -0.125 to 0.125
- value_scale: float32 [1024], P('tp'), may hold values from 0.5 to 2
- gate_scale: float32 [1024], P('tp'), may hold values from 0.5 to 2
- conv_taps: float32 [31, 1024], P(None, 'tp'), may hold values from -7 to 7
- chan_gain: float32 [1024], P('tp'), may hold values from 0.1 to 1.9
- mixout_weight: float32 [1024, 2048], P('tp', 'fs'), may hold values from -0.1875 to 0.1875
- mixout_scale: float32 [2048], P('fs'), may hold values from 0.5 to 2
- second_gain: float32 [2048], replicated, may hold values from 0.1 to 1.9
- up_weight: float32 [2048, 8192], P('fs', 'tp'), may hold values from -0.125 to 0.125
- up_scale: float32 [8192], P('tp'), may hold values from 0.5 to 2
- down_weight: float32 [8192, 2048], P('tp', 'fs'), may hold values from -0.0625 to 0.0625
- down_scale: float32 [2048], P('fs'), may hold values from 0.5 to 2
Outputs:
- layer_out: bfloat16 [4096, 2048], P(('rep', 'fs'))
The draws below stay inside these ranges and needn't reach their ends.
All inputs are finite; a program needn't handle non-finite values.
Results may differ from the reference program's by a relative error of at most 0.025.
Values may be sent and summed in bfloat16 or wider, within the bound.
A program may use at most 128 MiB of HBM per device.

```python
import math
import jax
import jax.numpy as jnp
from jax import lax

D = 2048
CHANNELS = 1024
FF = 8192
CONV_K = 31
SEQ_LEN = 128
TOKENS = 4096
N_TP = 2


def draw_conv_taps(key, part):
    first, second = jax.random.split(jax.random.fold_in(key, 11))
    channel = jnp.arange(CHANNELS).astype(jnp.float32)
    rise = jnp.exp(jnp.log(6.0) * channel / max(CHANNELS - 1, 1))
    base = jnp.clip(jax.random.normal(first, (CONV_K, CHANNELS), jnp.float32), -4.0, 4.0)
    rough = jax.random.uniform(second, (CHANNELS,), jnp.float32, 0.5, 1.5)
    return (base * CONV_K ** (-0.5) * rise * rough).astype(jnp.float32)


def levels(key, dims, cuts, low, high):
    def one(dim, blocks):
        heights = jax.random.uniform(jax.random.fold_in(jax.random.fold_in(key, 6), dim), (blocks,), jnp.float32, low / len(cuts), high / len(cuts))
        return jnp.repeat(jnp.exp(heights), dims[dim] // blocks).reshape((-1,) + (1,) * (len(dims) - dim - 1))

    level = one(*cuts[0])
    for cut in cuts[1:]:
        level = level * one(*cut)
    return level


def scatter_about(own_key, extent, scale, reach, cuts=(), kind=jnp.bfloat16):
    factor_of = levels(own_key, extent, cuts, -0.22, 0.18) if cuts else 1.0
    values = jax.random.normal(own_key, extent, jnp.float32) * scale * factor_of
    return jnp.minimum(jnp.maximum(values, -reach), reach).astype(kind)


def setup_inputs(seed: int = 0) -> dict:
    keys = jax.random.split(jax.random.key(seed), 16)
    tokens = scatter_about(keys[0], (TOKENS, D), 1.0, 6.0, ((0, 16),))
    first_gain = jnp.clip(1.0 + 0.18 * jax.random.normal(keys[1], (D,), jnp.float32), 0.1, 1.9)
    value_weight = scatter_about(keys[2], (D, CHANNELS), D ** -0.5, 0.125, ((0, 8), (1, 2)), jnp.float32)
    gate_weight = scatter_about(keys[3], (D, CHANNELS), D ** -0.5, 0.125, ((0, 8), (1, 2)), jnp.float32)
    value_scale = jnp.clip(jnp.exp(math.log(2.0) - 1.3862944 * jax.random.uniform(keys[4], (CHANNELS,), jnp.float32) ** levels(keys[4], (CHANNELS,), ((0, 2),), -0.2, 0.2)), 0.5, 2.0)
    gate_scale = jnp.clip(jnp.exp(math.log(2.0) - 1.3862944 * jax.random.uniform(keys[5], (CHANNELS,), jnp.float32) ** levels(keys[5], (CHANNELS,), ((0, 2),), -0.2, 0.2)), 0.5, 2.0)
    conv_taps = draw_conv_taps(jax.random.fold_in(keys[15], 71), 0)
    chan_gain = jnp.clip(1.0 + 0.18 * jax.random.normal(keys[7], (CHANNELS,), jnp.float32), 0.1, 1.9)
    mixout_weight = scatter_about(keys[8], (CHANNELS, D), CHANNELS ** -0.5, 0.1875, ((0, 2), (1, 8)), jnp.float32)
    mixout_scale = jnp.clip(jnp.exp(math.log(2.0) - 1.3862944 * jax.random.uniform(keys[9], (D,), jnp.float32) ** levels(keys[9], (D,), ((0, 8),), -0.2, 0.2)), 0.5, 2.0)
    second_gain = jnp.clip(1.0 + 0.18 * jax.random.normal(keys[10], (D,), jnp.float32), 0.1, 1.9)
    up_weight = scatter_about(keys[11], (D, FF), D ** -0.5, 0.125, ((0, 8), (1, 2)), jnp.float32)
    up_scale = jnp.clip(jnp.exp(math.log(2.0) - 1.3862944 * jax.random.uniform(keys[12], (FF,), jnp.float32) ** levels(keys[12], (FF,), ((0, 2),), -0.2, 0.2)), 0.5, 2.0)
    down_weight = scatter_about(keys[13], (FF, D), FF ** -0.5, 0.0625, ((0, 2), (1, 8)), jnp.float32)
    down_scale = jnp.clip(jnp.exp(math.log(2.0) - 1.3862944 * jax.random.uniform(keys[14], (D,), jnp.float32) ** levels(keys[14], (D,), ((0, 8),), -0.2, 0.2)), 0.5, 2.0)
    return {"tokens": tokens, "first_gain": first_gain, "value_weight": value_weight, "gate_weight": gate_weight, "value_scale": value_scale, "gate_scale": gate_scale, "conv_taps": conv_taps, "chan_gain": chan_gain, "mixout_weight": mixout_weight, "mixout_scale": mixout_scale, "second_gain": second_gain, "up_weight": up_weight, "up_scale": up_scale, "down_weight": down_weight, "down_scale": down_scale}


def rms_rows(rows, gain):
    values = rows.astype(jnp.float32)
    scaled = values * lax.rsqrt(lax.optimization_barrier(jnp.mean(values * values, axis=-1, keepdims=True)) + 1e-05)
    return (scaled * gain).astype(jnp.bfloat16)

def rounded(scale):
    return lax.optimization_barrier(scale.astype(jnp.bfloat16)).astype(jnp.float32)

def causal_conv(signal, taps):
    width = signal.shape[1]
    seqs = signal.reshape(-1, SEQ_LEN, width)
    result = lax.conv_general_dilated(seqs, taps[:, None, :], (1,), [(taps.shape[0] - 1, 0)], dimension_numbers=('NWC', 'WIO', 'NWC'), feature_group_count=width, precision=lax.Precision.HIGHEST)
    return result.reshape(signal.shape)

def block_sum(left, right, scale):
    inner = left.shape[1] // N_TP
    total = jnp.zeros((left.shape[0], right.shape[1]), jnp.float32)
    for block in range(N_TP):
        term = jnp.dot(left[:, block * inner:(block + 1) * inner], right[block * inner:(block + 1) * inner], preferred_element_type=jnp.float32) * scale
        total = total + lax.optimization_barrier(term.astype(jnp.bfloat16)).astype(jnp.float32)
    return total

def reference(tokens, first_gain, value_weight, gate_weight, value_scale, gate_scale, conv_taps, chan_gain, mixout_weight, mixout_scale, second_gain, up_weight, up_scale, down_weight, down_scale):
    normed = rms_rows(tokens, first_gain)
    value_sum = jnp.dot(normed, value_weight.astype(jnp.bfloat16), preferred_element_type=jnp.float32)
    gate_sum = jnp.dot(normed, gate_weight.astype(jnp.bfloat16), preferred_element_type=jnp.float32)
    glu = value_sum * rounded(value_scale) * jax.nn.sigmoid(gate_sum * rounded(gate_scale))
    conv = causal_conv(glu, conv_taps)
    mean = lax.optimization_barrier(jnp.mean(conv, axis=1, keepdims=True))
    centred = conv - mean
    var = lax.optimization_barrier(jnp.mean(centred * centred, axis=1, keepdims=True))
    mixed_in = jax.nn.silu(centred * lax.rsqrt(var + 1e-05) * chan_gain).astype(jnp.bfloat16)
    mix_sum = block_sum(mixed_in, mixout_weight.astype(jnp.bfloat16), rounded(mixout_scale))
    middle = (tokens.astype(jnp.float32) + mix_sum).astype(jnp.bfloat16)
    normed2 = rms_rows(middle, second_gain)
    up_sum = jnp.dot(normed2, up_weight.astype(jnp.bfloat16), preferred_element_type=jnp.float32)
    hidden = jnp.square(jax.nn.relu(up_sum * rounded(up_scale))).astype(jnp.bfloat16)
    down_sum = block_sum(hidden, down_weight.astype(jnp.bfloat16), rounded(down_scale))
    return (middle.astype(jnp.float32) + down_sum).astype(jnp.bfloat16)
```

```python
import jax
import jax.numpy as jnp
from jax import lax
from jax.experimental import pallas as pl
from jax.experimental.pallas import tpu as pltpu
from jax.sharding import PartitionSpec as P

SEQ_LEN = 128


def rms_rows(rows, gain):
    values = rows.astype(jnp.float32)
    scaled = values * lax.rsqrt(jnp.mean(values * values, axis=-1, keepdims=True) + 1e-05)
    return (scaled * gain).astype(jnp.bfloat16)


def causal_conv(signal, taps):
    width = signal.shape[1]
    seqs = signal.reshape(-1, SEQ_LEN, width)
    result = lax.conv_general_dilated(
        seqs,
        taps[:, None, :],
        (1,),
        [(taps.shape[0] - 1, 0)],
        dimension_numbers=("NWC", "WIO", "NWC"),
        feature_group_count=width,
        precision=lax.Precision.HIGHEST,
    )
    return result.reshape(signal.shape)


def on_device(
    tokens,
    first_gain,
    value_weight,
    gate_weight,
    value_scale,
    gate_scale,
    conv_taps,
    chan_gain,
    mixout_weight,
    mixout_scale,
    second_gain,
    up_weight,
    up_scale,
    down_weight,
    down_scale,
):
    normed = rms_rows(tokens, first_gain)
    count = normed.shape[0]
    width = value_weight.shape[1]
    columns = normed
    value_sum = jnp.dot(
        columns,
        lax.all_gather(value_weight.astype(jnp.bfloat16), "fs", axis=0, tiled=True),
        preferred_element_type=jnp.float32,
    )
    gate_sum = jnp.dot(
        columns,
        lax.all_gather(gate_weight.astype(jnp.bfloat16), "fs", axis=0, tiled=True),
        preferred_element_type=jnp.float32,
    )
    value_mult = value_scale.astype(jnp.bfloat16).astype(jnp.float32)
    gate_mult = gate_scale.astype(jnp.bfloat16).astype(jnp.float32)
    glu = value_sum * value_mult * jax.nn.sigmoid(gate_sum * gate_mult)
    conv = causal_conv(glu, conv_taps)
    total = width * lax.axis_size("tp")
    sums, squares = lax.psum((jnp.sum(conv, axis=1), jnp.sum(conv * conv, axis=1)), "tp")
    mean = sums / total
    var = squares / total - mean * mean
    centred = conv - mean[:, None]
    mixed_in = jax.nn.silu(centred * lax.rsqrt(var[:, None] + 1e-05) * chan_gain).astype(
        jnp.bfloat16
    )
    out_whole, out_mult = (
        lax.all_gather(mixout_weight.astype(jnp.bfloat16), "fs", axis=1, tiled=True),
        lax.all_gather(mixout_scale.astype(jnp.bfloat16), "fs", axis=0, tiled=True),
    )
    out_factor = out_mult.astype(jnp.float32)
    mix_term = jnp.dot(mixed_in, out_whole, preferred_element_type=jnp.float32) * out_factor
    mix_sum = lax.psum(mix_term.astype(jnp.bfloat16), "tp").astype(jnp.float32)
    middle = (tokens.astype(jnp.float32) + mix_sum).astype(jnp.bfloat16)
    normed2 = rms_rows(middle, second_gain)
    up_empty = jnp.zeros((count, up_weight.shape[1]), jnp.float32)
    piece = lax.all_gather(up_weight.astype(jnp.bfloat16), "fs", axis=0, tiled=True)
    columns = lax.slice_in_dim(normed2, 0, piece.shape[0], axis=1)
    up_sum = up_empty + jnp.dot(columns, piece, preferred_element_type=jnp.float32)
    up_mult = up_scale.astype(jnp.bfloat16).astype(jnp.float32)
    hidden = jnp.square(jax.nn.relu(up_sum * up_mult)).astype(jnp.bfloat16)
    down_whole, down_mult = (
        lax.all_gather(down_weight.astype(jnp.bfloat16), "fs", axis=1, tiled=True),
        lax.all_gather(down_scale.astype(jnp.bfloat16), "fs", axis=0, tiled=True),
    )
    down_factor = down_mult.astype(jnp.float32)
    down_term = jnp.dot(hidden, down_whole, preferred_element_type=jnp.float32) * down_factor
    down_sum = lax.psum(down_term.astype(jnp.bfloat16), "tp").astype(jnp.float32)
    return (middle.astype(jnp.float32) + down_sum).astype(jnp.bfloat16)


MESH = pl.DeviceIdType.MESH
F32, B16 = jnp.float32, jnp.bfloat16
LANES = 128


def aligned(index, step):
    return pl.ds(pl.multiple_of(index * step, step), step)


def flip(index, mask):
    value = index
    bit = 1
    while bit <= mask:
        if mask & bit:
            value = value + bit * (1 - 2 * ((index // bit) % 2))
        bit *= 2
    return value


def remote(src, dst, send_sem, recv_sem, target):
    return pltpu.make_async_remote_copy(
        src_ref=src,
        dst_ref=dst,
        send_sem=send_sem,
        recv_sem=recv_sem,
        device_id=target,
        device_id_type=MESH,
    )


class Exchange:
    def __init__(self, view, order, target, send, recv):
        self.view, self.order, self.target = view, order, target
        self.send, self.recv = send, recv
        self.stages = []

    def start(self):
        done = self.order[: len(self.stages)]
        mask = self.order[len(self.stages)]
        slots = [0]
        for one in done:
            slots += [s ^ one for s in slots]
        copies = []
        for s in slots:
            copy = remote(
                self.view(s, s), self.view(s, s ^ mask), self.send.at[s ^ mask], self.recv.at[s ^ mask], self.target(mask)
            )
            copy.start()
            copies.append((s ^ mask, copy))
        self.stages.append(copies)

    def land(self, stage):
        for _, copy in self.stages[stage]:
            copy.wait_recv()
        return [slot for slot, _ in self.stages[stage]]

    def close(self):
        for stage in self.stages:
            for _, copy in stage:
                copy.wait_send()


def rms(values, gain):
    scale = lax.rsqrt(jnp.mean(values * values, axis=1, keepdims=True) + 1e-05)
    return (values * scale * gain).astype(B16)


GATHER_ORDERS = ((2, 1, 4), (1, 2, 4), (4, 2, 1), (4, 1, 2))
REDUCE_ORDERS = ((4, 2, 1), (1, 4, 2), (2, 1, 4), (4, 1, 2), (1, 2, 4), (2, 4, 1), (4, 2, 1), (1, 4, 2))


def layer_kernel(
    tokens, first_gain, value_w, gate_w, value_scale, gate_scale, taps, chan_gain, mix_w, mix_scale, second_gain,
    up_w, up_scale, down_w, down_scale, out,
    value_in, gate_in, mix_in, up_in, down_in, x_tok, normed, value_all, gate_all, mix_all, up_cut, down_cut,
    up_all, down_all, padded, conv, row_stats, mixed, product, mix_send, mix_recv, mix_keep, half_send, half_recv,
    middle, ours, theirs, acc, hidden, part_send, part_recv, parts, land_a, land_b, land_c,
    load, tok_s, tok_r, w_s, w_r, m_s, m_r, a_s, a_r, st_s, st_r, mp_s, mp_r, mx_s, mx_r,
    g_s, g_r, gt_s, gt_r, p_s, p_r, r_s, r_r, o_s, o_r,
):
    n = 8
    here, rep, tp = lax.axis_index("fs"), lax.axis_index("rep"), lax.axis_index("tp")
    count, wide = tokens.shape
    half = count // 2
    chans = value_in.shape[1]
    hid = up_cut.shape[2]
    cols = mix_in.shape[1]
    depth = value_in.shape[0]
    seq = SEQ_LEN
    partner = {"tp": 1 - tp}
    across = {"rep": 1 - rep}
    corner = {"rep": 1 - rep, "tp": 1 - tp}

    def plane(mask):
        return {"fs": flip(here, mask)}

    def cube(mask):
        return across if mask == 4 else plane(mask)

    loads = [
        pltpu.make_async_copy(value_w.at[:, aligned(rep, chans)], value_in, load.at[0]),
        pltpu.make_async_copy(gate_w.at[:, aligned(rep, chans)], gate_in, load.at[1]),
        pltpu.make_async_copy(mix_w.at[aligned(rep, chans)], mix_in, load.at[2]),
        pltpu.make_async_copy(up_w.at[:, aligned(rep, 4 * hid)], up_in, load.at[3]),
        pltpu.make_async_copy(down_w.at[aligned(rep, 4 * hid)], down_in, load.at[4]),
    ]
    for copy in loads:
        copy.start()
    barrier = pltpu.get_barrier_semaphore()
    peers = [plane(k) for k in range(1, n)] + [partner, across, corner]
    for peer in peers:
        pl.semaphore_signal(barrier, inc=1, device_id=peer, device_id_type=MESH)
    loads[0].wait()
    value_all[here] = value_in[...].astype(B16)
    loads[1].wait()
    gate_all[here] = gate_in[...].astype(B16)
    pl.semaphore_wait(barrier, len(peers))

    closing = []

    own_rows = aligned(tp, half)
    tok = remote(tokens.at[own_rows], x_tok.at[own_rows], tok_s.at[0], tok_r.at[0], across)
    tok.start()
    closing.append(tok)

    piece = depth // 2

    def rows_of(ref, i):
        return lambda s, _: ref.at[flip(here, s), pl.ds(i * piece, piece)]

    first = [
        Exchange(rows_of(value_all, 0), (4, 2, 1), plane, w_s.at[0], w_r.at[0]),
        Exchange(rows_of(gate_all, 0), (4, 1, 2), plane, w_s.at[1], w_r.at[1]),
        Exchange(rows_of(value_all, 1), (4, 2, 1), plane, w_s.at[2], w_r.at[2]),
        Exchange(rows_of(gate_all, 1), (4, 2, 1), plane, w_s.at[3], w_r.at[3]),
    ]
    for one in first:
        one.start()

    loads[2].wait()
    factor = mix_scale[...].astype(B16).astype(F32)
    mix_all[here] = (mix_in[...].astype(B16).astype(F32) * factor).astype(B16)
    loads[3].wait()
    for j in range(4):
        up_cut[j] = up_in[:, j * hid : (j + 1) * hid].astype(B16)
    own = here % 4
    up_all[here] = up_in[:, aligned(own, hid)].astype(B16)

    sent = []

    def push(*items):
        for kind, s in items:
            to = flip(here, s)
            if kind == "u":
                copy = remote(up_cut.at[to % 4], up_all.at[here], a_s.at[s], a_r.at[s], {"fs": to})
            else:
                copy = remote(down_cut.at[to % 4], down_all.at[here], a_s.at[n + s], a_r.at[n + s], {"fs": to})
            copy.start()
            sent.append((kind, s, copy))

    def arrived(kind, slots):
        for one, s, copy in sent:
            if one == kind and s in slots:
                copy.wait_recv()

    push(("u", 4))

    def norm_block(src, at):
        def body(i, _):
            there = pl.ds(pl.multiple_of(i * 32, 32), 32)
            values = src[there].astype(F32)
            normed[pl.ds(pl.multiple_of(at * count + i * 32, 32), 32)] = rms(values, first_gain[...])
            return 0

        lax.fori_loop(0, count // 32, body, 0)

    norm_block(tokens, rep)
    for one in first:
        one.land(0)
        one.start()
    push(("u", 5))
    loads[4].wait()
    factor_d = down_scale[...].astype(B16).astype(F32)
    for j in range(4):
        block = down_in[j * hid : (j + 1) * hid].astype(B16).astype(F32) * factor_d
        down_cut[j] = block.astype(B16)
    down_all[here] = (down_in[aligned(own, hid)].astype(B16).astype(F32) * factor_d).astype(B16)

    tok.wait_recv()
    tok_on = remote(x_tok.at[own_rows], x_tok.at[own_rows], tok_s.at[1], tok_r.at[1], partner)
    tok_on.start()
    closing.append(tok_on)

    for one in first:
        one.land(1)
        one.start()
    second = [
        Exchange(rows_of(mix_all, 0), (4, 2, 1), plane, m_s.at[0], m_r.at[0]),
        Exchange(rows_of(mix_all, 1), (4, 1, 2), plane, m_s.at[1], m_r.at[1]),
    ]
    for one in second:
        one.start()
    push(("u", 6))
    tok_on.wait_recv()
    norm_block(x_tok, 1 - rep)
    for one in second:
        one.land(0)
        one.start()
    push(("u", 7))
    for one in first:
        one.land(2)
    for one in second:
        one.land(1)
        one.start()
    push(("u", 1), ("u", 2), ("u", 3), ("d", 1), ("d", 2), ("d", 3))

    value_mult = value_scale[:, aligned(rep, chans)].astype(B16).astype(F32)
    gate_mult = gate_scale[:, aligned(rep, chans)].astype(B16).astype(F32)
    wv = value_all[...].reshape(n * depth, chans)
    wg = gate_all[...].reshape(n * depth, chans)
    pad = padded.shape[1] - seq
    for b in range(padded.shape[0]):
        rows = normed[b * seq : (b + 1) * seq]
        value = jnp.dot(rows, wv, preferred_element_type=F32)
        gate = jnp.dot(rows, wg, preferred_element_type=F32)
        padded[b, :pad] = jnp.zeros((pad, chans), F32)
        padded[b, pad:] = value * value_mult * jax.nn.sigmoid(gate * gate_mult)

    n_taps = taps.shape[0]
    eye = lax.broadcasted_iota(jnp.int32, (seq, seq), 0) == lax.broadcasted_iota(jnp.int32, (seq, seq), 1)
    gain = chan_gain[:, aligned(rep, chans)]
    tap_rows = taps[:, aligned(rep, chans)]

    for b in range(padded.shape[0]):
        sums = jnp.zeros((seq, 1), F32)
        squares = jnp.zeros((seq, 1), F32)
        for lane in range(chans // LANES):
            at = slice(lane * LANES, (lane + 1) * LANES)
            total = jnp.zeros((seq, LANES), F32)
            start = pad - n_taps + 1
            for shift in range(8):
                offsets = [o for o in range(start, pad + 1) if o % 8 == shift]
                if not offsets:
                    continue
                low = offsets[0]
                span = offsets[-1] - low + seq
                window = padded[b, low : low + span, at]
                for o in offsets:
                    tap = tap_rows[o - start : o - start + 1, at]
                    total = total + tap * window[o - low : o - low + seq]
            conv[b, :, at] = total
            sums = sums + jnp.sum(total, axis=1, keepdims=True)
            squares = squares + jnp.sum(total * total, axis=1, keepdims=True)
        row_stats[0, b : b + 1] = jnp.sum(jnp.where(eye, sums, 0.0), axis=0, keepdims=True)
        row_stats[0, 4 + b : 5 + b] = jnp.sum(jnp.where(eye, squares, 0.0), axis=0, keepdims=True)

    stats = []
    for i, target in enumerate((partner, across, corner)):
        copy = remote(row_stats.at[0], row_stats.at[1 + i], st_s.at[i], st_r.at[i], target)
        copy.start()
        stats.append(copy)
    for copy in stats:
        copy.wait_recv()
    closing += stats
    both = row_stats[0] + row_stats[1] + row_stats[2] + row_stats[3]
    n_chans = chans * 4
    means = both[:4] / n_chans
    scales = lax.rsqrt(both[4:] / n_chans - means * means + 1e-05)
    for b in range(padded.shape[0]):
        mean = jnp.sum(jnp.where(eye, means[b : b + 1], 0.0), axis=1, keepdims=True)
        scale = jnp.sum(jnp.where(eye, scales[b : b + 1], 0.0), axis=1, keepdims=True)
        level = (conv[b] - mean) * scale * gain
        mixed[b * seq : (b + 1) * seq] = (level / (1.0 + jnp.exp(-level))).astype(B16)

    for one in second:
        one.land(2)

    def kept_rows(r, t):
        return pl.ds(pl.multiple_of(r * count + t * half, half), half)

    passes, hops = [], []
    for f in range(n):
        product[...] = jnp.dot(mixed[...], mix_all[f], preferred_element_type=F32)
        for r in range(2):
            mix_send[f, r] = product[kept_rows(r, 1 - tp)].astype(B16)
            mix_keep[f, r] = product[kept_rows(r, tp)]
        copy = remote(mix_send.at[f], mix_recv.at[f], mp_s.at[f], mp_r.at[f], partner)
        copy.start()
        passes.append(copy)
        if f >= 1:
            fold_pass(f - 1, passes, mix_keep, mix_recv, half_send, half_recv, mx_s, mx_r, across, rep, hops)
    fold_pass(n - 1, passes, mix_keep, mix_recv, half_send, half_recv, mx_s, mx_r, across, rep, hops)
    closing += passes + hops
    norm_sum = jnp.zeros((half, 1), F32)
    for f in range(n):
        at = slice(f * cols, (f + 1) * cols)
        hops[f].wait_recv()
        total = mix_keep[f, rep] + mix_recv[f, rep].astype(F32) + half_recv[f].astype(F32)
        block = (tokens[own_rows, at].astype(F32) + total).astype(B16)
        middle[:, at] = block
        wide_block = block.astype(F32)
        norm_sum = norm_sum + jnp.sum(wide_block * wide_block, axis=1, keepdims=True)
    scale2 = lax.rsqrt(norm_sum / wide + 1e-05)
    chunk = ours.shape[2]
    n_chunks = ours.shape[0]
    for q in range(n_chunks):
        at = slice(q * chunk, (q + 1) * chunk)
        ours[q, :half] = (middle[:, at].astype(F32) * scale2 * second_gain[:, at]).astype(B16)

    def slot_of(ref, q):
        return lambda s, to: ref.at[q, pl.ds(to * half, half)]

    gathers = [
        Exchange(slot_of(ours, q), GATHER_ORDERS[q % 4], cube, g_s.at[q], g_r.at[q]) for q in range(n_chunks)
    ]
    forwards = [[] for _ in gathers]

    def forward(q, slots):
        for s in slots:
            there = pl.ds(s * half, half)
            copy = remote(ours.at[q, there], theirs.at[q, there], gt_s.at[q, s], gt_r.at[q, s], partner)
            copy.start()
            forwards[q].append(copy)

    for one in gathers:
        one.start()
    for q in range(n_chunks):
        forward(q, [0])
    far = [("d", 4), ("d", 5), ("d", 6), ("d", 7)]
    push(*far[:1])
    for q, one in enumerate(gathers):
        slots = one.land(0)
        one.start()
        forward(q, slots)
    push(*far[1:2])
    for q, one in enumerate(gathers):
        slots = one.land(1)
        one.start()
        forward(q, slots)
    push(*far[2:])
    arrived("u", range(1, n))
    rows_all = n * half
    step = 256
    last_mult = up_scale[:, aligned(rep * 4 + own, hid)].astype(B16).astype(F32)
    for q, one in enumerate(gathers):
        forward(q, one.land(2))
        for copy in forwards[q]:
            copy.wait_recv()
        for side, ref in enumerate((ours, theirs)):
            def body(i, _, q=q, side=side, ref=ref):
                there = pl.ds(pl.multiple_of(i * step, step), step)
                into = pl.ds(pl.multiple_of(side * rows_all + i * step, step), step)
                w = up_all[q * (chunk // depth) : (q + 1) * (chunk // depth)].reshape(chunk, hid)
                value = jnp.dot(ref[q, there], w, preferred_element_type=F32)
                if q > 0:
                    value = value + acc[into]
                if q < n_chunks - 1:
                    acc[into] = value
                else:
                    value = jnp.maximum(value * last_mult, 0.0)
                    hidden[into] = (value * value).astype(B16)
                return 0

            lax.fori_loop(0, rows_all // step, body, 0)

    arrived("d", range(1, 4))
    near = here // 4

    def group(g):
        return (g + 4 * near) % n

    lands = (land_a, land_b, land_c)
    passed, flights, finals = [], [[] for _ in range(n)], []

    def multiply(g):
        w = down_all[group(g)]
        for side, ref in ((1, part_send), (0, parts)):
            def body(i, _, side=side, ref=ref):
                there = pl.ds(pl.multiple_of(i * step, step), step)
                from_rows = pl.ds(pl.multiple_of(side * rows_all + i * step, step), step)
                ref[g, there] = jnp.dot(hidden[from_rows], w, preferred_element_type=F32).astype(B16)
                return 0

            lax.fori_loop(0, rows_all // step, body, 0)
            if side == 1:
                copy = remote(part_send.at[g], part_recv.at[g], p_s.at[g], p_r.at[g], partner)
                copy.start()
                passed.append(copy)

    def rows(s):
        return slice(s * half, (s + 1) * half)

    def going(g, stage):
        order = REDUCE_ORDERS[g]
        kept = [s for s in range(n) if not any(s & m for m in order[:stage])]
        mask = order[stage]
        return [s for s in kept if s & mask], [s for s in kept if not s & mask], mask

    def ship(g, stage):
        leave, _, mask = going(g, stage)
        for i, s in enumerate(leave):
            sem = (0, 4, 6)[stage] + i
            copy = remote(
                parts.at[g, pl.ds(s * half, half)],
                lands[stage].at[g, pl.ds(i * half, half)],
                r_s.at[g, sem],
                r_r.at[g, sem],
                cube(mask),
            )
            copy.start()
            flights[g].append((stage, i, s ^ mask, copy))

    def begin(g):
        passed[g].wait_recv()
        leave, stay, _ = going(g, 0)
        for s in leave:
            there = rows(s)
            parts[g, there] = (parts[g, there].astype(F32) + part_recv[g, there].astype(F32)).astype(B16)
        ship(g, 0)

    def advance(g, stage):
        came = [(i, s) for at, i, s, copy in flights[g] if at == stage]
        for at, i, s, copy in flights[g]:
            if at == stage:
                copy.wait_recv()
        for i, s in came:
            there = rows(s)
            value = parts[g, there].astype(F32) + lands[stage][g, rows(i)].astype(F32)
            if stage == 0:
                value = value + part_recv[g, there].astype(F32)
            if stage < 2:
                parts[g, there] = value.astype(B16)
            else:
                at = aligned(group(g), cols)
                out[own_rows, at] = (middle[:, at].astype(F32) + value).astype(B16)
        if stage < 2:
            ship(g, stage + 1)
        else:
            at = aligned(group(g), cols)
            copy = remote(out.at[own_rows, at], out.at[own_rows, at], o_s.at[g], o_r.at[g], partner)
            copy.start()
            finals.append(copy)

    events = []
    for g in range(n):
        events += [(g, 0, g), (g + 1, 1, g), (g + 3, 2, g), (g + 5, 3, g), (g + 7, 4, g)]
    for _, kind, g in sorted(events, key=lambda e: (e[0], -e[1])):
        if kind == 0:
            if g == 4:
                arrived("d", range(4, n))
            multiply(g)
        elif kind == 1:
            begin(g)
        else:
            advance(g, kind - 2)

    for one in first + second + gathers:
        one.close()
    for some in forwards + [[c for _, _, c in sent], closing, passed, finals]:
        for copy in some:
            copy.wait_send()
    for some in flights:
        for _, _, _, copy in some:
            copy.wait_send()
    for copy in finals:
        copy.wait_recv()


def fold_pass(f, passes, mix_keep, mix_recv, half_send, half_recv, mx_s, mx_r, across, rep, hops):
    passes[f].wait_recv()
    half_send[f] = (mix_keep[f, 1 - rep] + mix_recv[f, 1 - rep].astype(F32)).astype(B16)
    copy = remote(half_send.at[f], half_recv.at[f], mx_s.at[f], mx_r.at[f], across)
    copy.start()
    hops.append(copy)


def layer_device(
    tokens, first_gain, value_weight, gate_weight, value_scale, gate_scale, conv_taps, chan_gain, mixout_weight,
    mixout_scale, second_gain, up_weight, up_scale, down_weight, down_scale,
):
    n = 8
    count, wide = tokens.shape
    depth, chans = value_weight.shape[0], value_weight.shape[1] // 2
    hid = up_weight.shape[1] // n
    cols = mixout_weight.shape[1]
    half = count // 2
    chunk = wide // 4
    rows = n * half
    vm, anywhere = pl.BlockSpec(memory_space=pltpu.VMEM), pl.BlockSpec(memory_space=pl.ANY)
    dma = pltpu.SemaphoreType.DMA

    def line(values):
        return values.reshape(1, -1)

    operands = [
        (tokens, vm),
        (line(first_gain), vm),
        (value_weight, anywhere),
        (gate_weight, anywhere),
        (line(value_scale), vm),
        (line(gate_scale), vm),
        (conv_taps, vm),
        (line(chan_gain), vm),
        (mixout_weight, anywhere),
        (line(mixout_scale), vm),
        (line(second_gain), vm),
        (up_weight, anywhere),
        (line(up_scale), vm),
        (down_weight, anywhere),
        (line(down_scale), vm),
    ]
    seqs = 2 * count // SEQ_LEN
    scratch = [
        ((depth, chans), F32),
        ((depth, chans), F32),
        ((chans, cols), F32),
        ((depth, 4 * hid), F32),
        ((4 * hid, cols), F32),
        ((count, wide), B16),
        ((2 * count, wide), B16),
        ((n, depth, chans), B16),
        ((n, depth, chans), B16),
        ((n, chans, cols), B16),
        ((4, depth, hid), B16),
        ((4, hid, cols), B16),
        ((n, depth, hid), B16),
        ((n, hid, cols), B16),
        ((seqs, SEQ_LEN + 32, chans), F32),
        ((seqs, SEQ_LEN, chans), F32),
        ((4, 8, SEQ_LEN), F32),
        ((2 * count, chans), B16),
        ((2 * count, cols), F32),
        ((n, 2, half, cols), B16),
        ((n, 2, half, cols), B16),
        ((n, 2, half, cols), F32),
        ((n, half, cols), B16),
        ((n, half, cols), B16),
        ((half, wide), B16),
        ((4, rows, chunk), B16),
        ((4, rows, chunk), B16),
        ((2 * rows, hid), F32),
        ((2 * rows, hid), B16),
        ((n, rows, cols), B16),
        ((n, rows, cols), B16),
        ((n, rows, cols), B16),
        ((n, 4 * half, cols), B16),
        ((n, 2 * half, cols), B16),
        ((n, half, cols), B16),
    ]
    sems = [(5,), (2,), (2,), (4, n), (4, n), (2, n), (2, n), (2 * n,), (2 * n,), (3,), (3,), (n,), (n,), (n,), (n,)]
    sems += [(4, n), (4, n), (4, n), (4, n), (n,), (n,), (n, n), (n, n), (n,), (n,)]
    return pl.pallas_call(
        layer_kernel,
        out_shape=jax.ShapeDtypeStruct((count, wide), B16),
        in_specs=[spec for _, spec in operands],
        out_specs=vm,
        scratch_shapes=[pltpu.VMEM(shape, kind) for shape, kind in scratch] + [dma(shape) for shape in sems],
        compiler_params=pltpu.CompilerParams(
            collective_id=0, has_side_effects=True, vmem_limit_bytes=60 * 1024 * 1024
        ),
    )(*[array for array, _ in operands])


def solution(mesh):
    placed = (
        P(("rep", "fs"), None),
        P(),
        P("fs", "tp"),
        P("fs", "tp"),
        P("tp"),
        P("tp"),
        P(None, "tp"),
        P("tp"),
        P("tp", "fs"),
        P("fs"),
        P(),
        P("fs", "tp"),
        P("tp"),
        P("tp", "fs"),
        P("fs"),
    )
    fits = mesh.shape["rep"] == 2 and mesh.shape["tp"] == 2 and mesh.shape["fs"] == 8
    return jax.shard_map(
        layer_device if fits else on_device,
        mesh=mesh,
        in_specs=placed,
        out_specs=P(("rep", "fs"), None),
        check_vma=False,
    )
```

```python
import jax
import jax.numpy as jnp
from jax import lax
from jax.experimental import pallas as pl
from jax.experimental.pallas import tpu as pltpu
from jax.sharding import PartitionSpec as P

SEQ_LEN = 128


def rms_rows(rows, gain):
    values = rows.astype(jnp.float32)
    scaled = values * lax.rsqrt(jnp.mean(values * values, axis=-1, keepdims=True) + 1e-05)
    return (scaled * gain).astype(jnp.bfloat16)


def causal_conv(signal, taps):
    width = signal.shape[1]
    seqs = signal.reshape(-1, SEQ_LEN, width)
    result = lax.conv_general_dilated(
        seqs,
        taps[:, None, :],
        (1,),
        [(taps.shape[0] - 1, 0)],
        dimension_numbers=("NWC", "WIO", "NWC"),
        feature_group_count=width,
        precision=lax.Precision.HIGHEST,
    )
    return result.reshape(signal.shape)


def on_device(
    tokens,
    first_gain,
    value_weight,
    gate_weight,
    value_scale,
    gate_scale,
    conv_taps,
    chan_gain,
    mixout_weight,
    mixout_scale,
    second_gain,
    up_weight,
    up_scale,
    down_weight,
    down_scale,
):
    normed = rms_rows(tokens, first_gain)
    count = normed.shape[0]
    width = value_weight.shape[1]
    columns = normed
    value_sum = jnp.dot(
        columns,
        lax.all_gather(value_weight.astype(jnp.bfloat16), "fs", axis=0, tiled=True),
        preferred_element_type=jnp.float32,
    )
    gate_sum = jnp.dot(
        columns,
        lax.all_gather(gate_weight.astype(jnp.bfloat16), "fs", axis=0, tiled=True),
        preferred_element_type=jnp.float32,
    )
    value_mult = value_scale.astype(jnp.bfloat16).astype(jnp.float32)
    gate_mult = gate_scale.astype(jnp.bfloat16).astype(jnp.float32)
    glu = value_sum * value_mult * jax.nn.sigmoid(gate_sum * gate_mult)
    conv = causal_conv(glu, conv_taps)
    total = width * lax.axis_size("tp")
    sums, squares = lax.psum((jnp.sum(conv, axis=1), jnp.sum(conv * conv, axis=1)), "tp")
    mean = sums / total
    var = squares / total - mean * mean
    centred = conv - mean[:, None]
    mixed_in = jax.nn.silu(centred * lax.rsqrt(var[:, None] + 1e-05) * chan_gain).astype(
        jnp.bfloat16
    )
    out_whole, out_mult = (
        lax.all_gather(mixout_weight.astype(jnp.bfloat16), "fs", axis=1, tiled=True),
        lax.all_gather(mixout_scale.astype(jnp.bfloat16), "fs", axis=0, tiled=True),
    )
    out_factor = out_mult.astype(jnp.float32)
    mix_term = jnp.dot(mixed_in, out_whole, preferred_element_type=jnp.float32) * out_factor
    mix_sum = lax.psum(mix_term.astype(jnp.bfloat16), "tp").astype(jnp.float32)
    middle = (tokens.astype(jnp.float32) + mix_sum).astype(jnp.bfloat16)
    normed2 = rms_rows(middle, second_gain)
    up_empty = jnp.zeros((count, up_weight.shape[1]), jnp.float32)
    piece = lax.all_gather(up_weight.astype(jnp.bfloat16), "fs", axis=0, tiled=True)
    columns = lax.slice_in_dim(normed2, 0, piece.shape[0], axis=1)
    up_sum = up_empty + jnp.dot(columns, piece, preferred_element_type=jnp.float32)
    up_mult = up_scale.astype(jnp.bfloat16).astype(jnp.float32)
    hidden = jnp.square(jax.nn.relu(up_sum * up_mult)).astype(jnp.bfloat16)
    down_whole, down_mult = (
        lax.all_gather(down_weight.astype(jnp.bfloat16), "fs", axis=1, tiled=True),
        lax.all_gather(down_scale.astype(jnp.bfloat16), "fs", axis=0, tiled=True),
    )
    down_factor = down_mult.astype(jnp.float32)
    down_term = jnp.dot(hidden, down_whole, preferred_element_type=jnp.float32) * down_factor
    down_sum = lax.psum(down_term.astype(jnp.bfloat16), "tp").astype(jnp.float32)
    return (middle.astype(jnp.float32) + down_sum).astype(jnp.bfloat16)


MESH = pl.DeviceIdType.MESH
F32, B16 = jnp.float32, jnp.bfloat16
LANES = 128


def aligned(index, step):
    return pl.ds(pl.multiple_of(index * step, step), step)


def flip(index, mask):
    value = index
    bit = 1
    while bit <= mask:
        if mask & bit:
            value = value + bit * (1 - 2 * ((index // bit) % 2))
        bit *= 2
    return value


def remote(src, dst, send_sem, recv_sem, target):
    return pltpu.make_async_remote_copy(
        src_ref=src,
        dst_ref=dst,
        send_sem=send_sem,
        recv_sem=recv_sem,
        device_id=target,
        device_id_type=MESH,
    )


class Exchange:
    def __init__(self, view, order, target, send, recv):
        self.view, self.order, self.target = view, order, target
        self.send, self.recv = send, recv
        self.stages = []

    def start(self):
        done = self.order[: len(self.stages)]
        mask = self.order[len(self.stages)]
        slots = [0]
        for one in done:
            slots += [s ^ one for s in slots]
        copies = []
        for s in slots:
            copy = remote(
                self.view(s, s), self.view(s, s ^ mask), self.send.at[s ^ mask], self.recv.at[s ^ mask], self.target(mask)
            )
            copy.start()
            copies.append((s ^ mask, copy))
        self.stages.append(copies)

    def land(self, stage):
        for _, copy in self.stages[stage]:
            copy.wait_recv()
        return [slot for slot, _ in self.stages[stage]]

    def close(self):
        for stage in self.stages:
            for _, copy in stage:
                copy.wait_send()


def rms(values, gain):
    scale = lax.rsqrt(jnp.mean(values * values, axis=1, keepdims=True) + 1e-05)
    return (values * scale * gain).astype(B16)


INNER = {'u': (0, 8, 8, 8, 1, 2, 4, 13), 'd': (0, 14, 15, 16, 31, 35, 38, 38)}
OUTER = {'u': (0, 8, 8, 8, 1, 2, 24, 13), 'd': (0, 14, 15, 16, 35, 36, 38, 38)}
SECOND_AT = (2, 4, 8)
FIRST_ORDERS = ((4, 2, 1), (4, 1, 2), (4, 2, 1), (4, 2, 1))
SECOND_ORDERS = ((4, 2, 1), (4, 1, 2))
GATHER_ORDERS = ((2, 1, 4), (1, 2, 4), (4, 2, 1), (4, 1, 2))
REDUCE_ORDERS = ((4, 2, 1), (1, 4, 2), (4, 1, 2), (2, 1, 4), (1, 2, 4), (4, 1, 2), (2, 4, 1), (1, 2, 4))
TIMES = ((0.0, 1.5), (3.0, 1.5), (11.0, 1.75), (16.0, 1.9), (23.0, 1.8))


def layer_kernel(
    tokens, first_gain, value_w, gate_w, value_scale, gate_scale, taps, chan_gain, mix_w, mix_scale, second_gain,
    up_w, up_scale, down_w, down_scale, out,
    value_in, gate_in, mix_in, up_in, down_in, x_tok, normed, value_all, gate_all, mix_all, up_cut, down_cut,
    up_all, down_all, padded, conv, row_stats, mixed, product, mix_send, mix_recv, mix_keep, half_send, half_recv,
    middle, ours, theirs, acc, hidden, part_recv, land_a, land_b, land_c,
    load, tok_s, tok_r, w_s, w_r, m_s, m_r, a_s, a_r, st_s, st_r, mp_s, mp_r, mx_s, mx_r,
    g_s, g_r, gt_s, gt_r, p_s, p_r, r_s, r_r, o_s, o_r,
):
    n = 8
    here, rep, tp = lax.axis_index("fs"), lax.axis_index("rep"), lax.axis_index("tp")
    count, wide = tokens.shape
    half = count // 2
    chans = value_in.shape[1]
    hid = up_cut.shape[2]
    cols = mix_in.shape[1]
    depth = value_in.shape[0]
    seq = SEQ_LEN
    partner = {"tp": 1 - tp}
    across = {"rep": 1 - rep}
    corner = {"rep": 1 - rep, "tp": 1 - tp}

    def plane(mask):
        return {"fs": flip(here, mask)}

    def cube(mask):
        return across if mask == 4 else plane(mask)

    loads = [
        pltpu.make_async_copy(value_w.at[:, aligned(rep, chans)], value_in, load.at[0]),
        pltpu.make_async_copy(gate_w.at[:, aligned(rep, chans)], gate_in, load.at[1]),
        pltpu.make_async_copy(mix_w.at[aligned(rep, chans)], mix_in, load.at[2]),
        pltpu.make_async_copy(up_w.at[:, aligned(rep, 4 * hid)], up_in, load.at[3]),
        pltpu.make_async_copy(down_w.at[aligned(rep, 4 * hid)], down_in, load.at[4]),
    ]
    for copy in loads:
        copy.start()
    barrier = pltpu.get_barrier_semaphore()
    peers = [plane(k) for k in range(1, n)] + [partner, across, corner]
    for peer in peers:
        pl.semaphore_signal(barrier, inc=1, device_id=peer, device_id_type=MESH)
    loads[0].wait()
    value_all[here] = value_in[...].astype(B16)
    loads[1].wait()
    gate_all[here] = gate_in[...].astype(B16)
    pl.semaphore_wait(barrier, len(peers))

    closing = []

    own_rows = aligned(tp, half)
    tok = remote(tokens.at[own_rows], x_tok.at[own_rows], tok_s.at[0], tok_r.at[0], across)
    tok.start()
    closing.append(tok)

    piece = depth // 2

    def rows_of(ref, i):
        return lambda s, _: ref.at[flip(here, s), pl.ds(i * piece, piece)]

    first = [
        Exchange(rows_of(value_all, 0), FIRST_ORDERS[0], plane, w_s.at[0], w_r.at[0]),
        Exchange(rows_of(gate_all, 0), FIRST_ORDERS[1], plane, w_s.at[1], w_r.at[1]),
        Exchange(rows_of(value_all, 1), FIRST_ORDERS[2], plane, w_s.at[2], w_r.at[2]),
        Exchange(rows_of(gate_all, 1), FIRST_ORDERS[3], plane, w_s.at[3], w_r.at[3]),
    ]
    for one in first:
        one.start()

    loads[2].wait()
    factor = mix_scale[...].astype(B16).astype(F32)
    mix_all[here] = (mix_in[...].astype(B16).astype(F32) * factor).astype(B16)
    loads[3].wait()
    for j in range(4):
        up_cut[j] = up_in[:, j * hid : (j + 1) * hid].astype(B16)
    own = here % 4
    up_all[here] = up_in[:, aligned(own, hid)].astype(B16)

    def block_copy(kind, s):
        to = flip(here, s)
        if kind == "u":
            return remote(up_cut.at[to % 4], up_all.at[here], a_s.at[s], a_r.at[s], {"fs": to})
        return remote(down_cut.at[to % 4], down_all.at[here], a_s.at[n + s], a_r.at[n + s], {"fs": to})

    layer = here // 2
    inner = jnp.logical_and(layer > 0, layer < 3)

    point = [0]

    def push():
        at = point[0]
        point[0] += 1
        mine = [(kind, s) for kind in "ud" for s in range(1, n) if INNER[kind][s] == at]
        theirs = [(kind, s) for kind in "ud" for s in range(1, n) if OUTER[kind][s] == at]
        always = [one for one in mine if one in theirs]
        for one in always:
            block_copy(*one).start()
        for side, items in ((inner, mine), (jnp.logical_not(inner), theirs)):
            items = [one for one in items if one not in always]
            if items:
                @pl.when(side)
                def _(items=items):
                    for one in items:
                        block_copy(*one).start()
        if at == SECOND_AT[0]:
            for one in second:
                one.start()
        for stage in range(2):
            if at == SECOND_AT[stage + 1]:
                for one in second:
                    one.land(stage)
                    one.start()

    def arrived(kind, slots):
        for s in slots:
            block_copy(kind, s).wait_recv()

    def norm_block(src, at):
        def body(i, _):
            there = pl.ds(pl.multiple_of(i * 32, 32), 32)
            values = src[there].astype(F32)
            normed[pl.ds(pl.multiple_of(at * count + i * 32, 32), 32)] = rms(values, first_gain[...])
            return 0

        lax.fori_loop(0, count // 32, body, 0)

    second = [
        Exchange(rows_of(mix_all, 0), SECOND_ORDERS[0], plane, m_s.at[0], m_r.at[0]),
        Exchange(rows_of(mix_all, 1), SECOND_ORDERS[1], plane, m_s.at[1], m_r.at[1]),
    ]
    push()
    loads[4].wait()
    factor_d = down_scale[...].astype(B16).astype(F32)
    for j in range(4):
        block = down_in[j * hid : (j + 1) * hid].astype(B16).astype(F32) * factor_d
        down_cut[j] = block.astype(B16)
    down_all[here] = (down_in[aligned(own, hid)].astype(B16).astype(F32) * factor_d).astype(B16)
    norm_block(tokens, rep)
    for one in first:
        one.land(0)
        one.start()
    push()

    tok.wait_recv()
    tok_on = remote(x_tok.at[own_rows], x_tok.at[own_rows], tok_s.at[1], tok_r.at[1], partner)
    tok_on.start()
    closing.append(tok_on)
    for one in first:
        one.land(1)
        one.start()
    push()
    tok_on.wait_recv()
    norm_block(x_tok, 1 - rep)
    push()
    for one in first:
        one.land(2)
    push()

    value_mult = value_scale[:, aligned(rep, chans)].astype(B16).astype(F32)
    gate_mult = gate_scale[:, aligned(rep, chans)].astype(B16).astype(F32)
    wv = value_all[...].reshape(n * depth, chans)
    wg = gate_all[...].reshape(n * depth, chans)
    pad = padded.shape[1] - seq
    for b in range(padded.shape[0]):
        rows = normed[b * seq : (b + 1) * seq]
        value = jnp.dot(rows, wv, preferred_element_type=F32)
        gate = jnp.dot(rows, wg, preferred_element_type=F32)
        padded[b, :pad] = jnp.zeros((pad, chans), F32)
        padded[b, pad:] = value * value_mult * jax.nn.sigmoid(gate * gate_mult)
        push()

    n_taps = taps.shape[0]
    eye = lax.broadcasted_iota(jnp.int32, (seq, seq), 0) == lax.broadcasted_iota(jnp.int32, (seq, seq), 1)
    gain = chan_gain[:, aligned(rep, chans)]
    tap_rows = taps[:, aligned(rep, chans)]

    for b in range(padded.shape[0]):
        sums = jnp.zeros((seq, 1), F32)
        squares = jnp.zeros((seq, 1), F32)
        for lane in range(chans // LANES):
            at = slice(lane * LANES, (lane + 1) * LANES)
            total = jnp.zeros((seq, LANES), F32)
            start = pad - n_taps + 1
            for shift in range(8):
                offsets = [o for o in range(start, pad + 1) if o % 8 == shift]
                if not offsets:
                    continue
                low = offsets[0]
                span = offsets[-1] - low + seq
                window = padded[b, low : low + span, at]
                for o in offsets:
                    tap = tap_rows[o - start : o - start + 1, at]
                    total = total + tap * window[o - low : o - low + seq]
            conv[b, :, at] = total
            sums = sums + jnp.sum(total, axis=1, keepdims=True)
            squares = squares + jnp.sum(total * total, axis=1, keepdims=True)
        row_stats[0, b : b + 1] = jnp.sum(jnp.where(eye, sums, 0.0), axis=0, keepdims=True)
        row_stats[0, 4 + b : 5 + b] = jnp.sum(jnp.where(eye, squares, 0.0), axis=0, keepdims=True)
        push()

    stats = []
    for i, target in enumerate((partner, across, corner)):
        copy = remote(row_stats.at[0], row_stats.at[1 + i], st_s.at[i], st_r.at[i], target)
        copy.start()
        stats.append(copy)
    for copy in stats:
        copy.wait_recv()
    push()
    closing += stats
    both = row_stats[0] + row_stats[1] + row_stats[2] + row_stats[3]
    n_chans = chans * 4
    means = both[:4] / n_chans
    scales = lax.rsqrt(both[4:] / n_chans - means * means + 1e-05)
    for b in range(padded.shape[0]):
        mean = jnp.sum(jnp.where(eye, means[b : b + 1], 0.0), axis=1, keepdims=True)
        scale = jnp.sum(jnp.where(eye, scales[b : b + 1], 0.0), axis=1, keepdims=True)
        level = (conv[b] - mean) * scale * gain
        mixed[b * seq : (b + 1) * seq] = (level / (1.0 + jnp.exp(-level))).astype(B16)

    for one in second:
        one.land(2)

    def kept_rows(r, t):
        return pl.ds(pl.multiple_of(r * count + t * half, half), half)

    passes, hops = [], []
    for f in range(n):
        product[...] = jnp.dot(mixed[...], mix_all[f], preferred_element_type=F32)
        for r in range(2):
            mix_send[f, r] = product[kept_rows(r, 1 - tp)].astype(B16)
            mix_keep[f, r] = product[kept_rows(r, tp)]
        copy = remote(mix_send.at[f], mix_recv.at[f], mp_s.at[f], mp_r.at[f], partner)
        copy.start()
        passes.append(copy)
        push()
        if f >= 1:
            fold_pass(f - 1, passes, mix_keep, mix_recv, half_send, half_recv, mx_s, mx_r, across, rep, hops)
    fold_pass(n - 1, passes, mix_keep, mix_recv, half_send, half_recv, mx_s, mx_r, across, rep, hops)
    closing += passes + hops
    norm_sum = jnp.zeros((half, 1), F32)
    for f in range(n):
        at = slice(f * cols, (f + 1) * cols)
        hops[f].wait_recv()
        total = mix_keep[f, rep] + mix_recv[f, rep].astype(F32) + half_recv[f].astype(F32)
        block = (tokens[own_rows, at].astype(F32) + total).astype(B16)
        middle[:, at] = block
        wide_block = block.astype(F32)
        norm_sum = norm_sum + jnp.sum(wide_block * wide_block, axis=1, keepdims=True)
        push()
    scale2 = lax.rsqrt(norm_sum / wide + 1e-05)
    chunk = ours.shape[2]
    n_chunks = ours.shape[0]
    for q in range(n_chunks):
        at = slice(q * chunk, (q + 1) * chunk)
        ours[q, :half] = (middle[:, at].astype(F32) * scale2 * second_gain[:, at]).astype(B16)

    def slot_of(ref, q):
        return lambda s, to: ref.at[q, pl.ds(to * half, half)]

    gathers = [
        Exchange(slot_of(ours, q), GATHER_ORDERS[q % 4], cube, g_s.at[q], g_r.at[q]) for q in range(n_chunks)
    ]
    forwards = [[] for _ in gathers]

    def forward(q, slots):
        for s in slots:
            there = pl.ds(s * half, half)
            copy = remote(ours.at[q, there], theirs.at[q, there], gt_s.at[q, s], gt_r.at[q, s], partner)
            copy.start()
            forwards[q].append(copy)

    for one in gathers:
        one.start()
    for q in range(n_chunks):
        forward(q, [0])
    push()
    for q, one in enumerate(gathers):
        slots = one.land(0)
        one.start()
        forward(q, slots)
        push()
    for q, one in enumerate(gathers):
        slots = one.land(1)
        one.start()
        forward(q, slots)
        push()
    arrived("u", range(1, n))
    rows_all = n * half
    step = 1024
    last_mult = up_scale[:, aligned(rep * 4 + own, hid)].astype(B16).astype(F32)
    for q, one in enumerate(gathers):
        forward(q, one.land(2))
        for copy in forwards[q]:
            copy.wait_recv()
        push()
        for side, ref in enumerate((ours, theirs)):
            def body(i, _, q=q, side=side, ref=ref):
                there = pl.ds(pl.multiple_of(i * step, step), step)
                into = pl.ds(pl.multiple_of(side * rows_all + i * step, step), step)
                w = up_all[q * (chunk // depth) : (q + 1) * (chunk // depth)].reshape(chunk, hid)
                value = jnp.dot(ref[q, there], w, preferred_element_type=F32)
                if q > 0:
                    value = value + acc[into]
                if q < n_chunks - 1:
                    acc[into] = value
                else:
                    value = jnp.maximum(value * last_mult, 0.0)
                    hidden[into] = (value * value).astype(B16)
                return 0

            lax.fori_loop(0, rows_all // step, body, 0)

    arrived("d", range(1, 4))
    near = here // 4

    def group(g):
        return (g + 4 * near) % n

    lands = (land_a, land_b, land_c)
    passed, flights, finals = [], [[] for _ in range(n)], []

    for one in gathers:
        one.close()
    for some in forwards:
        for copy in some:
            copy.wait_send()
    per = chunk // cols

    def block_at(ref, g, there):
        return ref.at[g // per, there, pl.ds((g % per) * cols, cols)]

    def multiply(g):
        w = down_all[group(g)]
        for side, ref in ((1, theirs), (0, ours)):
            def body(i, _, side=side, ref=ref):
                there = pl.ds(pl.multiple_of(i * step, step), step)
                from_rows = pl.ds(pl.multiple_of(side * rows_all + i * step, step), step)
                block_at(ref, g, there)[...] = jnp.dot(hidden[from_rows], w, preferred_element_type=F32).astype(B16)
                return 0

            lax.fori_loop(0, rows_all // step, body, 0)
            if side == 1:
                copy = remote(block_at(theirs, g, pl.ds(0, rows_all)), part_recv.at[g], p_s.at[g], p_r.at[g], partner)
                copy.start()
                passed.append(copy)

    def rows(s):
        return pl.ds(s * half, half)

    def going(g, stage):
        order = REDUCE_ORDERS[g]
        kept = [s for s in range(n) if not any(s & m for m in order[:stage])]
        mask = order[stage]
        return [s for s in kept if s & mask], [s for s in kept if not s & mask], mask

    def ship(g, stage):
        leave, _, mask = going(g, stage)
        for i, s in enumerate(leave):
            sem = (0, 4, 6)[stage] + i
            copy = remote(
                block_at(ours, g, pl.ds(s * half, half)),
                lands[stage].at[g, pl.ds(i * half, half)],
                r_s.at[g, sem],
                r_r.at[g, sem],
                cube(mask),
            )
            copy.start()
            flights[g].append((stage, i, s ^ mask, copy))

    def begin(g):
        passed[g].wait_recv()
        leave, stay, _ = going(g, 0)
        for s in leave:
            there = rows(s)
            part = block_at(ours, g, there)
            part[...] = (part[...].astype(F32) + part_recv[g, there].astype(F32)).astype(B16)
        ship(g, 0)

    def advance(g, stage):
        came = [(i, s) for at, i, s, copy in flights[g] if at == stage]
        for at, i, s, copy in flights[g]:
            if at == stage:
                copy.wait_recv()
        for i, s in came:
            there = rows(s)
            part = block_at(ours, g, there)
            value = part[...].astype(F32) + lands[stage][g, rows(i)].astype(F32)
            if stage == 0:
                value = value + part_recv[g, there].astype(F32)
            if stage < 2:
                part[...] = value.astype(B16)
            else:
                at = aligned(group(g), cols)
                out[own_rows, at] = (middle[:, at].astype(F32) + value).astype(B16)
        if stage < 2:
            ship(g, stage + 1)
        else:
            at = aligned(group(g), cols)
            copy = remote(out.at[own_rows, at], out.at[own_rows, at], o_s.at[g], o_r.at[g], partner)
            copy.start()
            finals.append(copy)

    events = [(at + pace * g, -kind, g) for kind, (at, pace) in enumerate(TIMES) for g in range(n)]
    for _, kind, g in sorted(events):
        kind = -kind
        if kind == 0:
            if g == 4:
                arrived("d", range(4, n))
            multiply(g)
            push()
        elif kind == 1:
            begin(g)
        else:
            advance(g, kind - 2)

    for one in first + second:
        one.close()
    for kind in "ud":
        for s in range(1, n):
            block_copy(kind, s).wait_send()
    for some in [closing, passed, finals]:
        for copy in some:
            copy.wait_send()
    for some in flights:
        for _, _, _, copy in some:
            copy.wait_send()
    for copy in finals:
        copy.wait_recv()


def fold_pass(f, passes, mix_keep, mix_recv, half_send, half_recv, mx_s, mx_r, across, rep, hops):
    passes[f].wait_recv()
    half_send[f] = (mix_keep[f, 1 - rep] + mix_recv[f, 1 - rep].astype(F32)).astype(B16)
    copy = remote(half_send.at[f], half_recv.at[f], mx_s.at[f], mx_r.at[f], across)
    copy.start()
    hops.append(copy)


def layer_device(
    tokens, first_gain, value_weight, gate_weight, value_scale, gate_scale, conv_taps, chan_gain, mixout_weight,
    mixout_scale, second_gain, up_weight, up_scale, down_weight, down_scale,
):
    n = 8
    count, wide = tokens.shape
    depth, chans = value_weight.shape[0], value_weight.shape[1] // 2
    hid = up_weight.shape[1] // n
    cols = mixout_weight.shape[1]
    half = count // 2
    chunk = wide // 4
    rows = n * half
    vm, anywhere = pl.BlockSpec(memory_space=pltpu.VMEM), pl.BlockSpec(memory_space=pl.ANY)
    dma = pltpu.SemaphoreType.DMA

    def line(values):
        return values.reshape(1, -1)

    operands = [
        (tokens, vm),
        (line(first_gain), vm),
        (value_weight, anywhere),
        (gate_weight, anywhere),
        (line(value_scale), vm),
        (line(gate_scale), vm),
        (conv_taps, vm),
        (line(chan_gain), vm),
        (mixout_weight, anywhere),
        (line(mixout_scale), vm),
        (line(second_gain), vm),
        (up_weight, anywhere),
        (line(up_scale), vm),
        (down_weight, anywhere),
        (line(down_scale), vm),
    ]
    seqs = 2 * count // SEQ_LEN
    scratch = [
        ((depth, chans), F32),
        ((depth, chans), F32),
        ((chans, cols), F32),
        ((depth, 4 * hid), F32),
        ((4 * hid, cols), F32),
        ((count, wide), B16),
        ((2 * count, wide), B16),
        ((n, depth, chans), B16),
        ((n, depth, chans), B16),
        ((n, chans, cols), B16),
        ((4, depth, hid), B16),
        ((4, hid, cols), B16),
        ((n, depth, hid), B16),
        ((n, hid, cols), B16),
        ((seqs, SEQ_LEN + 32, chans), F32),
        ((seqs, SEQ_LEN, chans), F32),
        ((4, 8, SEQ_LEN), F32),
        ((2 * count, chans), B16),
        ((2 * count, cols), F32),
        ((n, 2, half, cols), B16),
        ((n, 2, half, cols), B16),
        ((n, 2, half, cols), F32),
        ((n, half, cols), B16),
        ((n, half, cols), B16),
        ((half, wide), B16),
        ((4, rows, chunk), B16),
        ((4, rows, chunk), B16),
        ((2 * rows, hid), F32),
        ((2 * rows, hid), B16),
        ((n, rows, cols), B16),
        ((n, 4 * half, cols), B16),
        ((n, 2 * half, cols), B16),
        ((n, half, cols), B16),
    ]
    sems = [(5,), (2,), (2,), (4, n), (4, n), (2, n), (2, n), (2 * n,), (2 * n,), (3,), (3,), (n,), (n,), (n,), (n,)]
    sems += [(4, n), (4, n), (4, n), (4, n), (n,), (n,), (n, n), (n, n), (n,), (n,)]
    return pl.pallas_call(
        layer_kernel,
        out_shape=jax.ShapeDtypeStruct((count, wide), B16),
        in_specs=[spec for _, spec in operands],
        out_specs=vm,
        scratch_shapes=[pltpu.VMEM(shape, kind) for shape, kind in scratch] + [dma(shape) for shape in sems],
        compiler_params=pltpu.CompilerParams(
            collective_id=0, has_side_effects=True, vmem_limit_bytes=63 * 1024 * 1024
        ),
    )(*[array for array, _ in operands])


def solution(mesh):
    placed = (
        P(("rep", "fs"), None),
        P(),
        P("fs", "tp"),
        P("fs", "tp"),
        P("tp"),
        P("tp"),
        P(None, "tp"),
        P("tp"),
        P("tp", "fs"),
        P("fs"),
        P(),
        P("fs", "tp"),
        P("tp"),
        P("tp", "fs"),
        P("fs"),
    )
    fits = mesh.shape["rep"] == 2 and mesh.shape["tp"] == 2 and mesh.shape["fs"] == 8
    return jax.shard_map(
        layer_device if fits else on_device,
        mesh=mesh,
        in_specs=placed,
        out_specs=P(("rep", "fs"), None),
        check_vma=False,
    )
```

```python
import jax
import jax.numpy as jnp
from jax import lax
from jax.experimental import pallas as pl
from jax.experimental.pallas import tpu as pltpu
from jax.sharding import PartitionSpec as P

SEQ_LEN = 128


def rms_rows(rows, gain):
    values = rows.astype(jnp.float32)
    scaled = values * lax.rsqrt(jnp.mean(values * values, axis=-1, keepdims=True) + 1e-05)
    return (scaled * gain).astype(jnp.bfloat16)


def causal_conv(signal, taps):
    width = signal.shape[1]
    seqs = signal.reshape(-1, SEQ_LEN, width)
    result = lax.conv_general_dilated(
        seqs,
        taps[:, None, :],
        (1,),
        [(taps.shape[0] - 1, 0)],
        dimension_numbers=("NWC", "WIO", "NWC"),
        feature_group_count=width,
        precision=lax.Precision.HIGHEST,
    )
    return result.reshape(signal.shape)


def on_device(
    tokens,
    first_gain,
    value_weight,
    gate_weight,
    value_scale,
    gate_scale,
    conv_taps,
    chan_gain,
    mixout_weight,
    mixout_scale,
    second_gain,
    up_weight,
    up_scale,
    down_weight,
    down_scale,
):
    normed = rms_rows(tokens, first_gain)
    count = normed.shape[0]
    width = value_weight.shape[1]
    columns = normed
    value_sum = jnp.dot(
        columns,
        lax.all_gather(value_weight.astype(jnp.bfloat16), "fs", axis=0, tiled=True),
        preferred_element_type=jnp.float32,
    )
    gate_sum = jnp.dot(
        columns,
        lax.all_gather(gate_weight.astype(jnp.bfloat16), "fs", axis=0, tiled=True),
        preferred_element_type=jnp.float32,
    )
    value_mult = value_scale.astype(jnp.bfloat16).astype(jnp.float32)
    gate_mult = gate_scale.astype(jnp.bfloat16).astype(jnp.float32)
    glu = value_sum * value_mult * jax.nn.sigmoid(gate_sum * gate_mult)
    conv = causal_conv(glu, conv_taps)
    total = width * lax.axis_size("tp")
    sums, squares = lax.psum((jnp.sum(conv, axis=1), jnp.sum(conv * conv, axis=1)), "tp")
    mean = sums / total
    var = squares / total - mean * mean
    centred = conv - mean[:, None]
    mixed_in = jax.nn.silu(centred * lax.rsqrt(var[:, None] + 1e-05) * chan_gain).astype(
        jnp.bfloat16
    )
    out_whole, out_mult = (
        lax.all_gather(mixout_weight.astype(jnp.bfloat16), "fs", axis=1, tiled=True),
        lax.all_gather(mixout_scale.astype(jnp.bfloat16), "fs", axis=0, tiled=True),
    )
    out_factor = out_mult.astype(jnp.float32)
    mix_term = jnp.dot(mixed_in, out_whole, preferred_element_type=jnp.float32) * out_factor
    mix_sum = lax.psum(mix_term.astype(jnp.bfloat16), "tp").astype(jnp.float32)
    middle = (tokens.astype(jnp.float32) + mix_sum).astype(jnp.bfloat16)
    normed2 = rms_rows(middle, second_gain)
    up_empty = jnp.zeros((count, up_weight.shape[1]), jnp.float32)
    piece = lax.all_gather(up_weight.astype(jnp.bfloat16), "fs", axis=0, tiled=True)
    columns = lax.slice_in_dim(normed2, 0, piece.shape[0], axis=1)
    up_sum = up_empty + jnp.dot(columns, piece, preferred_element_type=jnp.float32)
    up_mult = up_scale.astype(jnp.bfloat16).astype(jnp.float32)
    hidden = jnp.square(jax.nn.relu(up_sum * up_mult)).astype(jnp.bfloat16)
    down_whole, down_mult = (
        lax.all_gather(down_weight.astype(jnp.bfloat16), "fs", axis=1, tiled=True),
        lax.all_gather(down_scale.astype(jnp.bfloat16), "fs", axis=0, tiled=True),
    )
    down_factor = down_mult.astype(jnp.float32)
    down_term = jnp.dot(hidden, down_whole, preferred_element_type=jnp.float32) * down_factor
    down_sum = lax.psum(down_term.astype(jnp.bfloat16), "tp").astype(jnp.float32)
    return (middle.astype(jnp.float32) + down_sum).astype(jnp.bfloat16)


MESH = pl.DeviceIdType.MESH
F32, B16 = jnp.float32, jnp.bfloat16
LANES = 128


def aligned(index, step):
    return pl.ds(pl.multiple_of(index * step, step), step)


def flip(index, mask):
    value = index
    bit = 1
    while bit <= mask:
        if mask & bit:
            value = value + bit * (1 - 2 * ((index // bit) % 2))
        bit *= 2
    return value


def remote(src, dst, send_sem, recv_sem, target):
    return pltpu.make_async_remote_copy(
        src_ref=src,
        dst_ref=dst,
        send_sem=send_sem,
        recv_sem=recv_sem,
        device_id=target,
        device_id_type=MESH,
    )


class Exchange:
    def __init__(self, view, order, target, send, recv):
        self.view, self.order, self.target = view, order, target
        self.send, self.recv = send, recv
        self.stages = []

    def start(self):
        done = self.order[: len(self.stages)]
        mask = self.order[len(self.stages)]
        slots = [0]
        for one in done:
            slots += [s ^ one for s in slots]
        copies = []
        for s in slots:
            copy = remote(
                self.view(s, s), self.view(s, s ^ mask), self.send.at[s ^ mask], self.recv.at[s ^ mask], self.target(mask)
            )
            copy.start()
            copies.append((s ^ mask, copy))
        self.stages.append(copies)

    def land(self, stage):
        for _, copy in self.stages[stage]:
            copy.wait_recv()
        return [slot for slot, _ in self.stages[stage]]

    def close(self):
        for stage in self.stages:
            for _, copy in stage:
                copy.wait_send()


def rms(values, gain):
    scale = lax.rsqrt(jnp.mean(values * values, axis=1, keepdims=True) + 1e-05)
    return (values * scale * gain).astype(B16)


INNER = {'u': (0, 8, 8, 8, 1, 2, 4, 13), 'd': (0, 14, 15, 16, 31, 35, 38, 38)}
OUTER = {'u': (0, 8, 8, 8, 1, 2, 24, 13), 'd': (0, 14, 15, 16, 35, 36, 38, 38)}
SECOND_AT = (2, 4, 6)
FIRST_ORDERS = ((4, 2, 1), (4, 1, 2), (4, 2, 1), (4, 2, 1))
SECOND_ORDERS = ((4, 2, 1), (4, 1, 2))
GATHER_ORDERS = ((2, 1, 4), (1, 2, 4), (4, 2, 1), (4, 1, 2))
REDUCE_ORDERS = ((4, 2, 1), (1, 4, 2), (4, 1, 2), (2, 1, 4), (1, 2, 4), (4, 1, 2), (2, 4, 1), (1, 2, 4))
TIMES = ((0.0, 1.5), (3.0, 1.5), (11.0, 1.75), (16.0, 1.9), (23.0, 1.8))


def layer_kernel(
    tokens, first_gain, value_w, gate_w, value_scale, gate_scale, taps, chan_gain, mix_w, mix_scale, second_gain,
    up_w, up_scale, down_w, down_scale, out,
    value_in, gate_in, mix_in, up_in, down_in, x_tok, normed, value_all, gate_all, mix_all, up_cut, down_cut,
    up_all, down_all, padded, conv, row_stats, mixed, product, mix_send, mix_recv, mix_keep, half_send, half_recv,
    middle, ours, theirs, acc, hidden, part_recv, land_a, land_b, land_c,
    load, tok_s, tok_r, w_s, w_r, m_s, m_r, a_s, a_r, st_s, st_r, mp_s, mp_r, mx_s, mx_r,
    g_s, g_r, gt_s, gt_r, p_s, p_r, r_s, r_r, o_s, o_r,
):
    n = 8
    here, rep, tp = lax.axis_index("fs"), lax.axis_index("rep"), lax.axis_index("tp")
    count, wide = tokens.shape
    half = count // 2
    chans = value_in.shape[1]
    hid = up_cut.shape[2]
    cols = mix_in.shape[1]
    depth = value_in.shape[0]
    seq = SEQ_LEN
    partner = {"tp": 1 - tp}
    across = {"rep": 1 - rep}
    corner = {"rep": 1 - rep, "tp": 1 - tp}

    def plane(mask):
        return {"fs": flip(here, mask)}

    def cube(mask):
        return across if mask == 4 else plane(mask)

    loads = [
        pltpu.make_async_copy(value_w.at[:, aligned(rep, chans)], value_in, load.at[0]),
        pltpu.make_async_copy(gate_w.at[:, aligned(rep, chans)], gate_in, load.at[1]),
        pltpu.make_async_copy(mix_w.at[aligned(rep, chans)], mix_in, load.at[2]),
        pltpu.make_async_copy(up_w.at[:, aligned(rep, 4 * hid)], up_in, load.at[3]),
        pltpu.make_async_copy(down_w.at[aligned(rep, 4 * hid)], down_in, load.at[4]),
    ]
    for copy in loads:
        copy.start()
    barrier = pltpu.get_barrier_semaphore()
    peers = [plane(k) for k in range(1, n)] + [partner, across, corner]
    for peer in peers:
        pl.semaphore_signal(barrier, inc=1, device_id=peer, device_id_type=MESH)
    loads[0].wait()
    value_all[here] = value_in[...].astype(B16)
    loads[1].wait()
    gate_all[here] = gate_in[...].astype(B16)
    pl.semaphore_wait(barrier, len(peers))

    closing = []

    own_rows = aligned(tp, half)
    tok = remote(tokens.at[own_rows], x_tok.at[own_rows], tok_s.at[0], tok_r.at[0], across)
    tok.start()
    closing.append(tok)

    piece = depth // 2

    def rows_of(ref, i):
        return lambda s, _: ref.at[flip(here, s), pl.ds(i * piece, piece)]

    first = [
        Exchange(rows_of(value_all, 0), FIRST_ORDERS[0], plane, w_s.at[0], w_r.at[0]),
        Exchange(rows_of(gate_all, 0), FIRST_ORDERS[1], plane, w_s.at[1], w_r.at[1]),
        Exchange(rows_of(value_all, 1), FIRST_ORDERS[2], plane, w_s.at[2], w_r.at[2]),
        Exchange(rows_of(gate_all, 1), FIRST_ORDERS[3], plane, w_s.at[3], w_r.at[3]),
    ]
    for one in first:
        one.start()

    loads[2].wait()
    factor = mix_scale[...].astype(B16).astype(F32)
    mix_all[here] = (mix_in[...].astype(B16).astype(F32) * factor).astype(B16)
    loads[3].wait()
    for j in range(4):
        up_cut[j] = up_in[:, j * hid : (j + 1) * hid].astype(B16)
    own = here % 4
    up_all[here] = up_in[:, aligned(own, hid)].astype(B16)

    def block_copy(kind, s):
        to = flip(here, s)
        if kind == "u":
            return remote(up_cut.at[to % 4], up_all.at[here], a_s.at[s], a_r.at[s], {"fs": to})
        return remote(down_cut.at[to % 4], down_all.at[here], a_s.at[n + s], a_r.at[n + s], {"fs": to})

    layer = here // 2
    inner = jnp.logical_and(layer > 0, layer < 3)

    point = [0]

    def push():
        at = point[0]
        point[0] += 1
        mine = [(kind, s) for kind in "ud" for s in range(1, n) if INNER[kind][s] == at]
        theirs = [(kind, s) for kind in "ud" for s in range(1, n) if OUTER[kind][s] == at]
        always = [one for one in mine if one in theirs]
        for one in always:
            block_copy(*one).start()
        for side, items in ((inner, mine), (jnp.logical_not(inner), theirs)):
            items = [one for one in items if one not in always]
            if items:
                @pl.when(side)
                def _(items=items):
                    for one in items:
                        block_copy(*one).start()
        if at == SECOND_AT[0]:
            for one in second:
                one.start()
        for stage in range(2):
            if at == SECOND_AT[stage + 1]:
                for one in second:
                    one.land(stage)
                    one.start()

    def arrived(kind, slots):
        for s in slots:
            block_copy(kind, s).wait_recv()

    def norm_block(src, at):
        def body(i, _):
            there = pl.ds(pl.multiple_of(i * 32, 32), 32)
            values = src[there].astype(F32)
            normed[pl.ds(pl.multiple_of(at * count + i * 32, 32), 32)] = rms(values, first_gain[...])
            return 0

        lax.fori_loop(0, count // 32, body, 0)

    second = [
        Exchange(rows_of(mix_all, 0), SECOND_ORDERS[0], plane, m_s.at[0], m_r.at[0]),
        Exchange(rows_of(mix_all, 1), SECOND_ORDERS[1], plane, m_s.at[1], m_r.at[1]),
    ]
    push()
    loads[4].wait()
    factor_d = down_scale[...].astype(B16).astype(F32)
    for j in range(4):
        block = down_in[j * hid : (j + 1) * hid].astype(B16).astype(F32) * factor_d
        down_cut[j] = block.astype(B16)
    down_all[here] = (down_in[aligned(own, hid)].astype(B16).astype(F32) * factor_d).astype(B16)
    norm_block(tokens, rep)
    for one in first:
        one.land(0)
        one.start()
    push()

    tok.wait_recv()
    tok_on = remote(x_tok.at[own_rows], x_tok.at[own_rows], tok_s.at[1], tok_r.at[1], partner)
    tok_on.start()
    closing.append(tok_on)
    for one in first:
        one.land(1)
        one.start()
    push()
    tok_on.wait_recv()
    norm_block(x_tok, 1 - rep)
    push()
    for one in first:
        one.land(2)
    push()

    value_mult = value_scale[:, aligned(rep, chans)].astype(B16).astype(F32)
    gate_mult = gate_scale[:, aligned(rep, chans)].astype(B16).astype(F32)
    wv = value_all[...].reshape(n * depth, chans)
    wg = gate_all[...].reshape(n * depth, chans)
    pad = padded.shape[1] - seq
    for b in range(padded.shape[0]):
        rows = normed[b * seq : (b + 1) * seq]
        value = jnp.dot(rows, wv, preferred_element_type=F32)
        gate = jnp.dot(rows, wg, preferred_element_type=F32)
        padded[b, :pad] = jnp.zeros((pad, chans), F32)
        padded[b, pad:] = value * value_mult * jax.nn.sigmoid(gate * gate_mult)
        push()

    n_taps = taps.shape[0]
    eye = lax.broadcasted_iota(jnp.int32, (seq, seq), 0) == lax.broadcasted_iota(jnp.int32, (seq, seq), 1)
    gain = chan_gain[:, aligned(rep, chans)]
    tap_rows = taps[:, aligned(rep, chans)]

    for b in range(padded.shape[0]):
        sums = jnp.zeros((seq, 1), F32)
        squares = jnp.zeros((seq, 1), F32)
        for lane in range(chans // LANES):
            at = slice(lane * LANES, (lane + 1) * LANES)
            total = jnp.zeros((seq, LANES), F32)
            start = pad - n_taps + 1
            for shift in range(8):
                offsets = [o for o in range(start, pad + 1) if o % 8 == shift]
                if not offsets:
                    continue
                low = offsets[0]
                span = offsets[-1] - low + seq
                window = padded[b, low : low + span, at]
                for o in offsets:
                    tap = tap_rows[o - start : o - start + 1, at]
                    total = total + tap * window[o - low : o - low + seq]
            conv[b, :, at] = total
            sums = sums + jnp.sum(total, axis=1, keepdims=True)
            squares = squares + jnp.sum(total * total, axis=1, keepdims=True)
        row_stats[0, b : b + 1] = jnp.sum(jnp.where(eye, sums, 0.0), axis=0, keepdims=True)
        row_stats[0, 4 + b : 5 + b] = jnp.sum(jnp.where(eye, squares, 0.0), axis=0, keepdims=True)
        push()

    stats = []
    for i, target in enumerate((partner, across, corner)):
        copy = remote(row_stats.at[0], row_stats.at[1 + i], st_s.at[i], st_r.at[i], target)
        copy.start()
        stats.append(copy)
    for copy in stats:
        copy.wait_recv()
    push()
    closing += stats
    both = row_stats[0] + row_stats[1] + row_stats[2] + row_stats[3]
    n_chans = chans * 4
    means = both[:4] / n_chans
    scales = lax.rsqrt(both[4:] / n_chans - means * means + 1e-05)
    for b in range(padded.shape[0]):
        mean = jnp.sum(jnp.where(eye, means[b : b + 1], 0.0), axis=1, keepdims=True)
        scale = jnp.sum(jnp.where(eye, scales[b : b + 1], 0.0), axis=1, keepdims=True)
        level = (conv[b] - mean) * scale * gain
        mixed[b * seq : (b + 1) * seq] = (level / (1.0 + jnp.exp(-level))).astype(B16)

    for one in second:
        one.land(2)

    def kept_rows(r, t):
        return pl.ds(pl.multiple_of(r * count + t * half, half), half)

    passes, hops = [], []
    for f in range(n):
        product[...] = jnp.dot(mixed[...], mix_all[f], preferred_element_type=F32)
        for r in range(2):
            mix_send[f, r] = product[kept_rows(r, 1 - tp)].astype(B16)
            mix_keep[f, r] = product[kept_rows(r, tp)]
        copy = remote(mix_send.at[f], mix_recv.at[f], mp_s.at[f], mp_r.at[f], partner)
        copy.start()
        passes.append(copy)
        push()
        if f >= 1:
            fold_pass(f - 1, passes, mix_keep, mix_recv, half_send, half_recv, mx_s, mx_r, across, rep, hops)
    fold_pass(n - 1, passes, mix_keep, mix_recv, half_send, half_recv, mx_s, mx_r, across, rep, hops)
    closing += passes + hops
    norm_sum = jnp.zeros((half, 1), F32)
    for f in range(n):
        at = slice(f * cols, (f + 1) * cols)
        hops[f].wait_recv()
        total = mix_keep[f, rep] + mix_recv[f, rep].astype(F32) + half_recv[f].astype(F32)
        block = (tokens[own_rows, at].astype(F32) + total).astype(B16)
        middle[:, at] = block
        wide_block = block.astype(F32)
        norm_sum = norm_sum + jnp.sum(wide_block * wide_block, axis=1, keepdims=True)
        push()
    scale2 = lax.rsqrt(norm_sum / wide + 1e-05)
    chunk = ours.shape[2]
    n_chunks = ours.shape[0]
    for q in range(n_chunks):
        at = slice(q * chunk, (q + 1) * chunk)
        ours[q, :half] = (middle[:, at].astype(F32) * scale2 * second_gain[:, at]).astype(B16)

    def slot_of(ref, q):
        return lambda s, to: ref.at[q, pl.ds(to * half, half)]

    gathers = [
        Exchange(slot_of(ours, q), GATHER_ORDERS[q % 4], cube, g_s.at[q], g_r.at[q]) for q in range(n_chunks)
    ]
    forwards = [[] for _ in gathers]

    def forward(q, slots):
        for s in slots:
            there = pl.ds(s * half, half)
            copy = remote(ours.at[q, there], theirs.at[q, there], gt_s.at[q, s], gt_r.at[q, s], partner)
            copy.start()
            forwards[q].append(copy)

    for one in gathers:
        one.start()
    for q in range(n_chunks):
        forward(q, [0])
    push()
    for q, one in enumerate(gathers):
        slots = one.land(0)
        one.start()
        forward(q, slots)
        push()
    for q, one in enumerate(gathers):
        slots = one.land(1)
        one.start()
        forward(q, slots)
        push()
    arrived("u", range(1, n))
    rows_all = n * half
    step = 1024
    last_mult = up_scale[:, aligned(rep * 4 + own, hid)].astype(B16).astype(F32)
    for q, one in enumerate(gathers):
        forward(q, one.land(2))
        for copy in forwards[q]:
            copy.wait_recv()
        push()
        for side, ref in enumerate((ours, theirs)):
            def body(i, _, q=q, side=side, ref=ref):
                there = pl.ds(pl.multiple_of(i * step, step), step)
                into = pl.ds(pl.multiple_of(side * rows_all + i * step, step), step)
                w = up_all[q * (chunk // depth) : (q + 1) * (chunk // depth)].reshape(chunk, hid)
                value = jnp.dot(ref[q, there], w, preferred_element_type=F32)
                if q > 0:
                    value = value + acc[into]
                if q < n_chunks - 1:
                    acc[into] = value
                else:
                    value = jnp.maximum(value * last_mult, 0.0)
                    hidden[into] = (value * value).astype(B16)
                return 0

            lax.fori_loop(0, rows_all // step, body, 0)

    arrived("d", range(1, 4))
    near = here // 4

    def group(g):
        return (g + 4 * near) % n

    lands = (land_a, land_b, land_c)
    passed, flights, finals = [], [[] for _ in range(n)], []

    for one in gathers:
        one.close()
    for some in forwards:
        for copy in some:
            copy.wait_send()
    per = chunk // cols

    def block_at(ref, g, there):
        return ref.at[g // per, there, pl.ds((g % per) * cols, cols)]

    def multiply(g):
        w = down_all[group(g)]
        for side, ref in ((1, theirs), (0, ours)):
            def body(i, _, side=side, ref=ref):
                there = pl.ds(pl.multiple_of(i * step, step), step)
                from_rows = pl.ds(pl.multiple_of(side * rows_all + i * step, step), step)
                block_at(ref, g, there)[...] = jnp.dot(hidden[from_rows], w, preferred_element_type=F32).astype(B16)
                return 0

            lax.fori_loop(0, rows_all // step, body, 0)
            if side == 1:
                copy = remote(block_at(theirs, g, pl.ds(0, rows_all)), part_recv.at[g], p_s.at[g], p_r.at[g], partner)
                copy.start()
                passed.append(copy)

    def rows(s):
        return pl.ds(s * half, half)

    def going(g, stage):
        order = REDUCE_ORDERS[g]
        kept = [s for s in range(n) if not any(s & m for m in order[:stage])]
        mask = order[stage]
        return [s for s in kept if s & mask], [s for s in kept if not s & mask], mask

    def ship(g, stage):
        leave, _, mask = going(g, stage)
        for i, s in enumerate(leave):
            sem = (0, 4, 6)[stage] + i
            copy = remote(
                block_at(ours, g, pl.ds(s * half, half)),
                lands[stage].at[g, pl.ds(i * half, half)],
                r_s.at[g, sem],
                r_r.at[g, sem],
                cube(mask),
            )
            copy.start()
            flights[g].append((stage, i, s ^ mask, copy))

    def begin(g):
        passed[g].wait_recv()
        leave, stay, _ = going(g, 0)
        for s in leave:
            there = rows(s)
            part = block_at(ours, g, there)
            part[...] = (part[...].astype(F32) + part_recv[g, there].astype(F32)).astype(B16)
        ship(g, 0)

    def advance(g, stage):
        came = [(i, s) for at, i, s, copy in flights[g] if at == stage]
        for at, i, s, copy in flights[g]:
            if at == stage:
                copy.wait_recv()
        for i, s in came:
            there = rows(s)
            part = block_at(ours, g, there)
            value = part[...].astype(F32) + lands[stage][g, rows(i)].astype(F32)
            if stage == 0:
                value = value + part_recv[g, there].astype(F32)
            if stage < 2:
                part[...] = value.astype(B16)
            else:
                at = aligned(group(g), cols)
                out[own_rows, at] = (middle[:, at].astype(F32) + value).astype(B16)
        if stage < 2:
            ship(g, stage + 1)
        else:
            at = aligned(group(g), cols)
            copy = remote(out.at[own_rows, at], out.at[own_rows, at], o_s.at[g], o_r.at[g], partner)
            copy.start()
            finals.append(copy)

    events = [(at + pace * g, -kind, g) for kind, (at, pace) in enumerate(TIMES) for g in range(n)]
    for _, kind, g in sorted(events):
        kind = -kind
        if kind == 0:
            if g == 4:
                arrived("d", range(4, n))
            multiply(g)
            push()
        elif kind == 1:
            begin(g)
        else:
            advance(g, kind - 2)

    for one in first + second:
        one.close()
    for kind in "ud":
        for s in range(1, n):
            block_copy(kind, s).wait_send()
    for some in [closing, passed, finals]:
        for copy in some:
            copy.wait_send()
    for some in flights:
        for _, _, _, copy in some:
            copy.wait_send()
    for copy in finals:
        copy.wait_recv()


def fold_pass(f, passes, mix_keep, mix_recv, half_send, half_recv, mx_s, mx_r, across, rep, hops):
    passes[f].wait_recv()
    half_send[f] = (mix_keep[f, 1 - rep] + mix_recv[f, 1 - rep].astype(F32)).astype(B16)
    copy = remote(half_send.at[f], half_recv.at[f], mx_s.at[f], mx_r.at[f], across)
    copy.start()
    hops.append(copy)


def layer_device(
    tokens, first_gain, value_weight, gate_weight, value_scale, gate_scale, conv_taps, chan_gain, mixout_weight,
    mixout_scale, second_gain, up_weight, up_scale, down_weight, down_scale,
):
    n = 8
    count, wide = tokens.shape
    depth, chans = value_weight.shape[0], value_weight.shape[1] // 2
    hid = up_weight.shape[1] // n
    cols = mixout_weight.shape[1]
    half = count // 2
    chunk = wide // 4
    rows = n * half
    vm, anywhere = pl.BlockSpec(memory_space=pltpu.VMEM), pl.BlockSpec(memory_space=pl.ANY)
    dma = pltpu.SemaphoreType.DMA

    def line(values):
        return values.reshape(1, -1)

    operands = [
        (tokens, vm),
        (line(first_gain), vm),
        (value_weight, anywhere),
        (gate_weight, anywhere),
        (line(value_scale), vm),
        (line(gate_scale), vm),
        (conv_taps, vm),
        (line(chan_gain), vm),
        (mixout_weight, anywhere),
        (line(mixout_scale), vm),
        (line(second_gain), vm),
        (up_weight, anywhere),
        (line(up_scale), vm),
        (down_weight, anywhere),
        (line(down_scale), vm),
    ]
    seqs = 2 * count // SEQ_LEN
    scratch = [
        ((depth, chans), F32),
        ((depth, chans), F32),
        ((chans, cols), F32),
        ((depth, 4 * hid), F32),
        ((4 * hid, cols), F32),
        ((count, wide), B16),
        ((2 * count, wide), B16),
        ((n, depth, chans), B16),
        ((n, depth, chans), B16),
        ((n, chans, cols), B16),
        ((4, depth, hid), B16),
        ((4, hid, cols), B16),
        ((n, depth, hid), B16),
        ((n, hid, cols), B16),
        ((seqs, SEQ_LEN + 32, chans), F32),
        ((seqs, SEQ_LEN, chans), F32),
        ((4, 8, SEQ_LEN), F32),
        ((2 * count, chans), B16),
        ((2 * count, cols), F32),
        ((n, 2, half, cols), B16),
        ((n, 2, half, cols), B16),
        ((n, 2, half, cols), F32),
        ((n, half, cols), B16),
        ((n, half, cols), B16),
        ((half, wide), B16),
        ((4, rows, chunk), B16),
        ((4, rows, chunk), B16),
        ((2 * rows, hid), F32),
        ((2 * rows, hid), B16),
        ((n, rows, cols), B16),
        ((n, 4 * half, cols), B16),
        ((n, 2 * half, cols), B16),
        ((n, half, cols), B16),
    ]
    sems = [(5,), (2,), (2,), (4, n), (4, n), (2, n), (2, n), (2 * n,), (2 * n,), (3,), (3,), (n,), (n,), (n,), (n,)]
    sems += [(4, n), (4, n), (4, n), (4, n), (n,), (n,), (n, n), (n, n), (n,), (n,)]
    return pl.pallas_call(
        layer_kernel,
        out_shape=jax.ShapeDtypeStruct((count, wide), B16),
        in_specs=[spec for _, spec in operands],
        out_specs=vm,
        scratch_shapes=[pltpu.VMEM(shape, kind) for shape, kind in scratch] + [dma(shape) for shape in sems],
        compiler_params=pltpu.CompilerParams(
            collective_id=0, has_side_effects=True, vmem_limit_bytes=63 * 1024 * 1024
        ),
    )(*[array for array, _ in operands])


def solution(mesh):
    placed = (
        P(("rep", "fs"), None),
        P(),
        P("fs", "tp"),
        P("fs", "tp"),
        P("tp"),
        P("tp"),
        P(None, "tp"),
        P("tp"),
        P("tp", "fs"),
        P("fs"),
        P(),
        P("fs", "tp"),
        P("tp"),
        P("tp", "fs"),
        P("fs"),
    )
    fits = mesh.shape["rep"] == 2 and mesh.shape["tp"] == 2 and mesh.shape["fs"] == 8
    return jax.shard_map(
        layer_device if fits else on_device,
        mesh=mesh,
        in_specs=placed,
        out_specs=P(("rep", "fs"), None),
        check_vma=False,
    )
```
